256 devices in a mesh: ra: 16 (over y, x), cb: 16 (over z, core).
Axes of the slice: x: 4, y: 4, z: 8, core: 2. Of those that a mesh axis runs over, the one named last changes fastest.
Arguments:
- hidden_states: bfloat16 [384, 4096], P(None, 'ra'), may hold values from -40 to 40
- gain_first: bfloat16 [4096], P('ra'), may hold values from 0.099609375 to 1.8984375
- gate_first: bfloat16 [4096, 11264], P('ra', 'cb'), may hold values from -0.09375 to 0.09375
- up_first: bfloat16 [4096, 11264], P('ra', 'cb'), may hold values from -0.09375 to 0.09375
- down_first: bfloat16 [11264, 4096], P('cb', 'ra'), may hold values from -0.0546875 to 0.0546875
- gain_second: bfloat16 [4096], P('ra'), may hold values from 0.099609375 to 1.8984375
- gate_second: bfloat16 [4096, 11264], P('ra', 'cb'), may hold values from -0.09375 to 0.09375
- up_second: bfloat16 [4096, 11264], P('ra', 'cb'), may hold values from -0.09375 to 0.09375
- down_second: bfloat16 [11264, 4096], P('cb', 'ra'), may hold values from -0.0546875 to 0.0546875
- gain_last: bfloat16 [4096], P('ra'), may hold values from 0.099609375 to 1.8984375
Outputs:
- closed: bfloat16 [384, 4096], P(None, 'ra')
The draws below stay inside these ranges and needn't reach their ends.
All inputs are finite; a program needn't handle non-finite values.
Results may differ from the reference program's by a relative error of at most 0.0098.
Values may be sent and summed in bfloat16 or wider, within the bound.
No kernel may reach another device: no remote copies, remote signals or barrier semaphores. Data moves between devices by JAX's collectives and lax.ppermute only.
A program may use at most 64 MiB of HBM per device.

```python
import math
import jax
import jax.numpy as jnp
from jax import lax

D = 4096
FF = 11264
TOKENS = 384


def draw_hidden_states(key, part):
    key_base, key_row, key_col = jax.random.split(key, 3)
    position = jnp.arange(D, dtype=jnp.float32) / D
    rough = jnp.exp(jax.random.uniform(key_col, (D,), jnp.float32, -0.35, 0.35))
    col_scale = 0.5 * jnp.exp(math.log(4.0) * position) * rough
    base = jnp.clip(jax.random.normal(key_base, (TOKENS, D), jnp.float32), -4.0, 4.0)
    row_scale = jnp.exp(jax.random.uniform(key_row, (TOKENS, 1), jnp.float32, math.log(0.3), math.log(3.0)))
    return (base * row_scale * col_scale[None, :]).astype(jnp.bfloat16)


def block_levels(own_key, dims, shards, low, top_value):
    loudness, own = 1.0, jax.random.fold_in(own_key, 6)
    for dim, blocks in shards:
        steps = jnp.exp(jax.random.uniform(jax.random.fold_in(own, dim), (blocks,), jnp.float32, low / len(shards), top_value / len(shards)))
        loudness = loudness * jnp.repeat(steps, dims[dim] // blocks).reshape([-1 if axis == dim else 1 for axis in range(len(dims))])
    return loudness


def centred(own_key, dims, spread, limit, shards=(), kind=jnp.bfloat16):
    result = jax.random.normal(own_key, dims, jnp.float32) * spread
    if len(shards) > 0:
        result = block_levels(own_key, dims, shards, -0.22, 0.18) * result
    return jnp.clip(result, min=-limit, max=limit).astype(kind)


def setup_inputs(seed: int = 0) -> dict:
    keys = jax.random.split(jax.random.key(seed), 11)
    hidden_states = draw_hidden_states(jax.random.fold_in(keys[10], 71), 0)
    gain_first = jnp.clip(1.0 + 0.18 * jax.random.normal(keys[1], (D,), jnp.float32), 0.099609375, 1.8984375).astype(jnp.bfloat16)
    gate_first = centred(keys[2], (D, FF), D ** -0.5, 0.09375, ((0, 16), (1, 16)))
    up_first = centred(keys[3], (D, FF), D ** -0.5, 0.09375, ((0, 16), (1, 16)))
    down_first = centred(keys[4], (FF, D), FF ** -0.5, 0.0546875, ((0, 16), (1, 16)))
    gain_second = jnp.clip(1.0 + 0.18 * jax.random.normal(keys[5], (D,), jnp.float32), 0.099609375, 1.8984375).astype(jnp.bfloat16)
    gate_second = centred(keys[6], (D, FF), D ** -0.5, 0.09375, ((0, 16), (1, 16)))
    up_second = centred(keys[7], (D, FF), D ** -0.5, 0.09375, ((0, 16), (1, 16)))
    down_second = centred(keys[8], (FF, D), FF ** -0.5, 0.0546875, ((0, 16), (1, 16)))
    gain_last = jnp.clip(1.0 + 0.18 * jax.random.normal(keys[9], (D,), jnp.float32), 0.099609375, 1.8984375).astype(jnp.bfloat16)
    return {"hidden_states": hidden_states, "gain_first": gain_first, "gate_first": gate_first, "up_first": up_first, "down_first": down_first, "gain_second": gain_second, "gate_second": gate_second, "up_second": up_second, "down_second": down_second, "gain_last": gain_last}


norm_eps = 1e-06
residual_weight = 0.25
branch_weight = 0.5

def half_step(stream, gain, w_gate, w_up, w_down):
    values = stream.astype(jnp.float32)
    scale = lax.rsqrt(lax.optimization_barrier(jnp.mean(values * values, axis=1, keepdims=True)) + norm_eps)
    normed = (values * gain.astype(jnp.float32)).astype(jnp.bfloat16)
    gate = jnp.dot(normed, w_gate, preferred_element_type=jnp.float32) * scale
    upper = jnp.dot(normed, w_up, preferred_element_type=jnp.float32) * scale
    hidden = (jax.nn.silu(gate) * upper).astype(jnp.bfloat16)
    branch = jnp.dot(hidden, w_down, preferred_element_type=jnp.float32)
    return (residual_weight * values + branch_weight * branch).astype(jnp.bfloat16)

def reference(hidden_states, gain_first, gate_first, up_first, down_first, gain_second, gate_second, up_second, down_second, gain_last):
    first = half_step(hidden_states, gain_first, gate_first, up_first, down_first)
    second = half_step(first, gain_second, gate_second, up_second, down_second)
    values = second.astype(jnp.float32)
    scale = lax.rsqrt(lax.optimization_barrier(jnp.mean(values * values, axis=1, keepdims=True)) + norm_eps)
    return (values * scale * gain_last.astype(jnp.float32)).astype(jnp.bfloat16)
```

```python
import jax
import jax.numpy as jnp
from jax import lax
from jax.sharding import PartitionSpec as P

D = 4096
norm_eps = 1e-06
residual_weight = 0.25
branch_weight = 0.5
bf16 = jnp.bfloat16
f32 = jnp.float32
CHUNK_ROWS = (24,)


def exchange(blocks, axis):
    return lax.all_to_all(blocks, axis, 0, 0, tiled=True)


def to_everyone(value, axis):
    length = lax.axis_size(axis)
    return exchange(jnp.broadcast_to(value[None], (length, *value.shape)), axis)


def in_two(value):
    high = value.astype(bf16)
    return high, (value - high.astype(f32)).astype(bf16)


def gate_up_parts(values, gain, weights, hidden):
    values = values.astype(f32)
    squares = jnp.sum(values * values, axis=1, keepdims=True)
    high, low = in_two(squares)
    normed = (values * gain.astype(f32)).astype(bf16)
    both = jnp.dot(normed, weights, preferred_element_type=f32).astype(bf16)
    lane = lax.broadcasted_iota(jnp.int32, both.shape, 1)
    both = jnp.where(lane == 2 * hidden, high, both)
    return jnp.where(lane == 2 * hidden + 1, low, both)


def hidden_of(blocks, hidden):
    total = jnp.sum(blocks.astype(f32), axis=0)
    squares = total[:, 2 * hidden : 2 * hidden + 1] + total[:, 2 * hidden + 1 : 2 * hidden + 2]
    scale = lax.rsqrt(squares / D + norm_eps)
    gate = total[:, :hidden] * scale
    upper = total[:, hidden : 2 * hidden] * scale
    return (jax.nn.silu(gate) * upper).astype(bf16)


def joined(w_gate, w_up):
    hidden = w_gate.shape[1]
    width = -(-(2 * hidden + 2) // 128) * 128
    return jnp.concatenate(
        [w_gate, w_up, jnp.zeros((w_gate.shape[0], width - 2 * hidden), bf16)], axis=1
    )


def half_step(streams, owned, gain, weights, w_down):
    hidden = w_down.shape[0]
    ra, cb = lax.axis_size("ra"), lax.axis_size("cb")
    parts = [gate_up_parts(s, gain, weights, hidden) for s in streams]
    parts = [exchange(p.reshape(ra, -1, p.shape[1]), "ra") for p in parts]
    hids = [to_everyone(hidden_of(p, hidden), "ra") for p in parts]
    branch = [
        jnp.dot(h.reshape(-1, hidden), w_down, preferred_element_type=f32).astype(bf16) for h in hids
    ]
    branch = [exchange(b.reshape(cb, -1, b.shape[1]), "cb") for b in branch]
    updated = [
        (residual_weight * o.astype(f32) + branch_weight * jnp.sum(b.astype(f32), axis=0)).astype(bf16)
        for o, b in zip(owned, branch)
    ]
    return [to_everyone(u, "cb").reshape(-1, u.shape[1]) for u in updated], updated


def body(
    hidden_states,
    gain_first,
    gate_first,
    up_first,
    down_first,
    gain_second,
    gate_second,
    up_second,
    down_second,
    gain_last,
):
    cb = lax.axis_size("cb")
    me = lax.axis_index("cb")
    streams, owned, start = [], [], 0
    for rows in CHUNK_ROWS:
        stream = hidden_states[start : start + rows * cb]
        streams.append(stream)
        owned.append(lax.dynamic_slice_in_dim(stream, me * rows, rows, 0))
        start += rows * cb
    first, owned = half_step(streams, owned, gain_first, joined(gate_first, up_first), down_first)
    second, _ = half_step(first, owned, gain_second, joined(gate_second, up_second), down_second)
    closed = []
    for s in second:
        values = s.astype(f32)
        squares = jnp.sum(to_everyone(jnp.sum(values * values, axis=1), "ra"), axis=0)
        scale = lax.rsqrt(squares / D + norm_eps)[:, None]
        closed.append((values * scale * gain_last.astype(f32)).astype(bf16))
    return jnp.concatenate(closed, axis=0)


def solution(mesh):
    return jax.shard_map(
        body,
        mesh=mesh,
        in_specs=(
            P(None, "ra"),
            P("ra"),
            P("ra", "cb"),
            P("ra", "cb"),
            P("cb", "ra"),
            P("ra"),
            P("ra", "cb"),
            P("ra", "cb"),
            P("cb", "ra"),
            P("ra"),
        ),
        out_specs=P(None, "ra"),
        check_vma=False,
    )
```

```python
import functools

import jax
import jax.numpy as jnp
from jax import lax
from jax.experimental import pallas as pl
from jax.experimental.pallas import tpu as pltpu
from jax.sharding import Mesh
from jax.sharding import PartitionSpec as P

norm_eps = 1e-06
residual_weight = 0.25
branch_weight = 0.5
bf16 = jnp.bfloat16
f32 = jnp.float32
TILE = 8
HALF = TILE // 2


def exchange(blocks, axis):
    return lax.all_to_all(blocks, axis, 0, 0, tiled=True)


def partner(value):
    return lax.ppermute(value, "c", [(0, 1), (1, 0)])


def rolled(value):
    return pltpu.roll(value, HALF, value.ndim - 2)


def first_half(shape):
    return lax.broadcasted_iota(jnp.int32, shape, len(shape) - 2) < HALF


def gate_up_kernel(group, hidden, x, gain, *refs):
    weights, out, padded = refs[:4], refs[4], refs[5]
    wide = out.shape[2]
    values = x[...].astype(f32)
    squares = jnp.sum(values * values, axis=1, keepdims=True)
    high = squares.astype(bf16).astype(f32)
    low = squares - high
    normed = (values * gain[...].astype(f32)).astype(bf16)
    lane = lax.broadcasted_iota(jnp.int32, (values.shape[0], wide), 1)
    padded[hidden:] = jnp.zeros((wide - hidden, padded.shape[1]), bf16)
    sums = []
    for weight in weights:
        padded[:hidden] = weight[...]
        sums.append(lax.dot_general(normed, padded[...], (((1,), (1,)), ((), ())), preferred_element_type=f32))
    sums[0] = jnp.where(lane == hidden, high, jnp.where(lane == hidden + 1, low, sums[0]))
    whole = group * TILE
    for k in range(2):
        gate, up = sums[2 * k], sums[2 * k + 1]
        at = 3 * TILE * k
        out[:, at : at + TILE] = gate[:whole].reshape(group, TILE, wide).astype(bf16)
        out[:, at + TILE : at + 2 * TILE] = up[:whole].reshape(group, TILE, wide).astype(bf16)
        gate = gate[whole:].reshape(group // 2, TILE, wide)
        up = up[whole:].reshape(group // 2, TILE, wide)
        first = first_half(gate.shape)
        even = jnp.where(first, gate, rolled(up))
        odd = jnp.where(first, rolled(gate), up)
        both = jnp.stack([even, odd], axis=1).reshape(group, TILE, wide)
        out[:, at + 2 * TILE : at + 3 * TILE] = both.astype(bf16)


def hidden_kernel(group, hidden, features, parts, out):
    total = parts[0].astype(f32)
    for k in range(1, group):
        total = total + parts[k].astype(f32)

    def gated(gate, up, scale):
        gate = gate * scale
        return gate * jax.nn.sigmoid(gate) * (up * scale)

    def scale_of(rows):
        squares = rows[:, hidden : hidden + 1] + rows[:, hidden + 1 : hidden + 2]
        return lax.rsqrt(squares / features + norm_eps)

    scale = scale_of(total[:TILE])
    mixed_scale = scale_of(total[2 * TILE : 3 * TILE])
    tiles, mixed = [], []
    for k in range(2):
        at = 3 * TILE * k
        tiles.append(gated(total[at : at + TILE], total[at + TILE : at + 2 * TILE], scale))
        both = total[at + 2 * TILE : at + 3 * TILE]
        mixed.append(gated(both, rolled(both), mixed_scale))
    tiles.append(jnp.where(first_half(mixed[0].shape), mixed[0], rolled(mixed[1])))
    rows = jnp.concatenate(tiles, axis=0)[:, :hidden].astype(bf16)
    for k in range(group):
        out[k] = rows


def down_kernel(group, hids, own, other, out):
    hidden, width = own.shape
    tiles = [
        hids[:, TILE * k : TILE * (k + 1)].astype(f32).reshape(group * TILE, hidden).astype(bf16) for k in range(3)
    ]
    dot = functools.partial(jnp.dot, preferred_element_type=f32)
    whole = dot(tiles[0], own[...]) + dot(tiles[1], other[...])
    mixed = dot(tiles[2], own[...]).reshape(group, TILE, width)
    mixed = mixed + rolled(dot(tiles[2], other[...]).reshape(group, TILE, width))
    mixed = mixed.reshape(group // 2, 2, TILE, width)
    even, odd = mixed[:, 0], mixed[:, 1]
    rest = jnp.where(first_half(even.shape), even, rolled(odd)).reshape(group // 2 * TILE, width)
    rows = jnp.concatenate([whole, rest], axis=0)
    out[...] = rows.reshape(out.shape).astype(bf16)


def update_kernel(group, parts, start, out, kept):
    total = parts[0].astype(f32)
    for k in range(1, group):
        total = total + parts[k].astype(f32)
    rows = (residual_weight * start[...].astype(f32) + branch_weight * total).astype(bf16)
    kept[...] = rows
    for k in range(group):
        out[k] = rows


def kernel_call(kernel, outs, scratch=()):
    inside = pl.BlockSpec(memory_space=pltpu.VMEM)
    many = isinstance(outs, list)

    def call(*args):
        return pl.pallas_call(
            kernel,
            out_shape=outs,
            in_specs=[inside] * len(args),
            out_specs=[inside] * len(outs) if many else inside,
            scratch_shapes=scratch,
            compiler_params=pltpu.CompilerParams(vmem_limit_bytes=12 * 2**20),
        )(*args)

    return call


def half_step(stream, start, gain, gates, ups, downs, features):
    ra, z = lax.axis_size("ra"), lax.axis_size("z")
    tokens, width = stream.shape
    hidden = gates[0].shape[0]
    wide = -(-(hidden + 2) // 128) * 128
    parts = kernel_call(
        functools.partial(gate_up_kernel, ra, hidden),
        jax.ShapeDtypeStruct((ra, 6 * TILE, wide), bf16),
        [pltpu.VMEM((wide, width), bf16)],
    )(stream, gain[None], gates[0], ups[0], gates[1], ups[1])
    parts = exchange(parts, "ra")
    hids = kernel_call(
        functools.partial(hidden_kernel, ra, hidden, features),
        jax.ShapeDtypeStruct((ra, 3 * TILE, hidden), bf16),
    )(parts)
    hids = exchange(hids, "ra")
    branch = kernel_call(
        functools.partial(down_kernel, ra),
        jax.ShapeDtypeStruct((z, tokens // z, width), bf16),
    )(hids, downs[0], downs[1])
    branch = exchange(branch, "z")
    updated, kept = kernel_call(
        functools.partial(update_kernel, z),
        [
            jax.ShapeDtypeStruct((z, tokens // z, width), bf16),
            jax.ShapeDtypeStruct((tokens // z, width), bf16),
        ],
    )(branch, start)
    return exchange(updated, "z").reshape(tokens, width), kept


def body(
    hidden_states,
    gain_first,
    gate_first,
    up_first,
    down_first,
    gain_second,
    gate_second,
    up_second,
    down_second,
    gain_last,
):
    features = hidden_states.shape[1] * lax.axis_size("ra")
    tokens = hidden_states.shape[0] // lax.axis_size("c")
    core = lax.axis_index("c")
    rows = tokens // lax.axis_size("z")
    stream = lax.dynamic_slice_in_dim(hidden_states, core * tokens, tokens, 0)
    start = lax.dynamic_slice_in_dim(hidden_states, core * tokens + lax.axis_index("z") * rows, rows, 0)
    pairs = [
        (w, partner(w)) for w in (gate_first.T, up_first.T, down_first, gate_second.T, up_second.T, down_second)
    ]
    first, start = half_step(stream, start, gain_first, *pairs[:3], features)
    second, _ = half_step(first, start, gain_second, *pairs[3:], features)
    other = partner(second)
    both = jnp.where(core == 0, jnp.concatenate([second, other], 0), jnp.concatenate([other, second], 0))
    values = both.astype(f32)
    squares = jnp.sum(values * values, axis=1)
    length = lax.axis_size("ra")
    squares = jnp.sum(exchange(jnp.broadcast_to(squares[None], (length, squares.shape[0])), "ra"), axis=0)
    scale = lax.rsqrt(squares / features + norm_eps)[:, None]
    return (values * scale * gain_last.astype(f32)).astype(bf16)


def solution(mesh):
    split = Mesh(mesh.devices.reshape(mesh.shape["ra"], -1, 2), ("ra", "z", "c"))
    cb = ("z", "c")
    return jax.shard_map(
        body,
        mesh=split,
        in_specs=(
            P(None, "ra"),
            P("ra"),
            P("ra", cb),
            P("ra", cb),
            P(cb, "ra"),
            P("ra"),
            P("ra", cb),
            P("ra", cb),
            P(cb, "ra"),
            P("ra"),
        ),
        out_specs=P(None, "ra"),
        check_vma=False,
    )
```

```python
import functools

import jax
import jax.numpy as jnp
from jax import lax
from jax.experimental import pallas as pl
from jax.experimental.pallas import tpu as pltpu
from jax.sharding import Mesh
from jax.sharding import PartitionSpec as P

norm_eps = 1e-06
residual_weight = 0.25
branch_weight = 0.5
bf16 = jnp.bfloat16
f32 = jnp.float32
TILE = 8
HALF = TILE // 2
LANES = 128


def exchange(blocks, axis):
    return lax.all_to_all(blocks, axis, 0, 0, tiled=True)


def partner(value):
    return lax.ppermute(value, "c", [(0, 1), (1, 0)])


def rolled(value):
    return pltpu.roll(value, HALF, value.ndim - 2)


def first_half(shape):
    return lax.broadcasted_iota(jnp.int32, shape, len(shape) - 2) < HALF


def sum_of(parts):
    total = parts[0].astype(f32)
    for k in range(1, parts.shape[0]):
        total = total + parts[k].astype(f32)
    return total


def row_of(gain):
    gain = gain[...].astype(f32)
    return jnp.concatenate([gain[k : k + 1] for k in range(gain.shape[0])], axis=1)


def sums_of(x, gain, both):
    values = x[...].astype(f32)
    normed = (values * row_of(gain)).astype(bf16)
    return values, lax.dot_general(normed, both[...], (((1,), (1,)), ((), ())), preferred_element_type=f32)


def put_together(gate, up, both):
    hidden = gate.shape[0]
    both[:hidden] = gate[...]
    both[hidden:] = up[...]


def first_own_kernel(x, gain, gate, up, out, both, near, done):
    hidden = gate.shape[0]
    copies = [
        pltpu.make_async_copy(gain, near, done.at[2]),
        pltpu.make_async_copy(gate, both.at[:hidden], done.at[0]),
        pltpu.make_async_copy(up, both.at[hidden:], done.at[1]),
    ]
    for copy in copies:
        copy.start()
    for copy in copies:
        copy.wait()
    out[...] = sums_of(x, near, both)[1].astype(bf16)


def own_kernel(x, gain, gate, up, out, both):
    put_together(gate, up, both)
    out[...] = sums_of(x, gain, both)[1].astype(bf16)


def dealt(own, other, group):
    own = own.reshape(group // 2, TILE, own.shape[1])
    other = other.reshape(own.shape)
    first = first_half(own.shape)
    even = jnp.where(first, own, rolled(other))
    odd = jnp.where(first, rolled(own), other)
    return jnp.stack([even, odd], axis=1).reshape(group, TILE, own.shape[2])


def packed_kernel(group, x, gain, gate, up, own, *refs):
    out, both = refs[-2:]
    put_together(gate, up, both)
    values, other = sums_of(x, gain, both)
    own = own[...].astype(f32)
    whole = group * TILE
    count = own.shape[1] // LANES
    rest = dealt(own[whole:], other[whole:], group)
    own = own[:whole].reshape(group, TILE, count * LANES)
    other = other[:whole].reshape(own.shape)
    for k in range(count):
        lanes = slice(k * LANES, (k + 1) * LANES)
        out[:, k] = own[:, :, lanes].astype(bf16)
        out[:, count + k] = other[:, :, lanes].astype(bf16)
        out[:, 2 * count + k] = rest[:, :, lanes].astype(bf16)
    squares = jnp.sum(values * values, axis=1, keepdims=True)
    high = squares.astype(bf16).astype(f32)
    lane = lax.broadcasted_iota(jnp.int32, (values.shape[0], LANES), 1)
    squares = jnp.where(lane % 2 == 0, high, squares - high)
    rest = dealt(squares[whole:], squares[whole:], group)
    squares = squares[:whole].reshape(group, TILE, LANES)
    lane = lax.broadcasted_iota(jnp.int32, squares.shape, 2)
    out[:, 3 * count] = jnp.where(lane < 2, squares, rest).astype(bf16)


def hidden_kernel(features, parts, out):
    group, count = parts.shape[0], parts.shape[1] // 3
    hidden = out.shape[2]
    total = sum_of(parts)
    rows = jnp.concatenate(
        [jnp.concatenate([total[count * t + k] for k in range(count)], axis=1) for t in range(3)], axis=0
    )
    squares = total[3 * count]
    whole = squares[:, 0:1] + squares[:, 1:2]
    rest = squares[:, 2:3] + squares[:, 3:4]
    scale = lax.rsqrt(jnp.concatenate([whole, whole, rest], axis=0) / features + norm_eps)
    gate = rows[:, :hidden] * scale
    up = pltpu.roll(rows, hidden, 1)[:, :hidden] * scale
    rows = (gate * jax.nn.sigmoid(gate) * up).astype(bf16)
    for k in range(group):
        out[k] = rows


def down_kernel(hids, own, other, out):
    group = hids.shape[0]
    hidden, width = own.shape
    tiles = [
        hids[:, TILE * k : TILE * (k + 1)].astype(f32).reshape(group * TILE, hidden).astype(bf16) for k in range(3)
    ]
    dot = functools.partial(jnp.dot, preferred_element_type=f32)
    whole = dot(tiles[0], own[...]) + dot(tiles[1], other[...])
    mixed = dot(tiles[2], own[...]).reshape(group, TILE, width)
    mixed = mixed + rolled(dot(tiles[2], other[...]).reshape(group, TILE, width))
    mixed = mixed.reshape(group // 2, 2, TILE, width)
    even, odd = mixed[:, 0], mixed[:, 1]
    rest = jnp.where(first_half(even.shape), even, rolled(odd)).reshape(group // 2 * TILE, width)
    rows = jnp.concatenate([whole, rest], axis=0)
    out[...] = rows.reshape(out.shape).astype(bf16)


def updated(parts, start):
    return (residual_weight * start[...].astype(f32) + branch_weight * sum_of(parts)).astype(bf16)


def update_kernel(parts, start, out, kept):
    rows = updated(parts, start)
    kept[...] = rows
    for k in range(out.shape[0]):
        out[k] = rows


def last_kernel(parts, start, kept, out):
    rows = updated(parts, start)
    kept[...] = rows
    values = rows.astype(f32)
    squares = jnp.sum(values * values, axis=1, keepdims=True)
    lane = lax.broadcasted_iota(jnp.int32, (TILE, LANES), 1)
    tile = jnp.zeros((TILE, LANES), f32)
    for t in range(rows.shape[0] // TILE):
        tile = jnp.where(lane == t, squares[TILE * t : TILE * (t + 1)], tile)
    for k in range(out.shape[0]):
        out[k] = tile


def closing_kernel(features, squares, rows, gain, out):
    total = sum_of(squares)
    count = rows.shape[0] // TILE
    total = jnp.concatenate([total[:, t : t + 1] for t in range(count)], axis=0)
    scale = lax.rsqrt(total / features + norm_eps)
    closed = (rows[...].astype(f32) * scale * row_of(gain)).astype(bf16)
    for k in range(out.shape[0]):
        out[k] = closed


def kernel_call(kernel, outs, scratch=(), outside=()):
    inside = pl.BlockSpec(memory_space=pltpu.VMEM)
    anywhere = pl.BlockSpec(memory_space=pltpu.HBM)
    many = isinstance(outs, list)

    def call(*args):
        return pl.pallas_call(
            kernel,
            out_shape=outs,
            in_specs=[anywhere if k in outside else inside for k in range(len(args))],
            out_specs=[inside] * len(outs) if many else inside,
            scratch_shapes=scratch,
            compiler_params=pltpu.CompilerParams(vmem_limit_bytes=12 * 2**20),
        )(*args)

    return call


def half_step(layer, stream, start, gain, gates, ups, downs, features):
    ra, z = lax.axis_size("ra"), lax.axis_size("z")
    tokens, width = stream.shape
    hidden = gates[0].shape[0]
    room = [pltpu.VMEM((2 * hidden, width), bf16)]
    struct = jax.ShapeDtypeStruct
    sums = struct((tokens, 2 * hidden), bf16)
    near = pltpu.VMEM(gain.shape, bf16)
    if layer == 0:
        call = kernel_call(first_own_kernel, sums, [*room, near, pltpu.SemaphoreType.DMA((3,))], (1, 2, 3))
    else:
        call = kernel_call(own_kernel, sums, room)
    mine = (gain, gates[0], ups[0])
    if layer == 0:
        mine = [pltpu.with_memory_space_constraint(w, pltpu.HBM) for w in mine]
    own = call(stream, *mine)
    slots = 3 * (2 * hidden // LANES) + 1
    parts = kernel_call(
        functools.partial(packed_kernel, ra), struct((ra, slots, TILE, LANES), bf16), room
    )(stream, gain, gates[1], ups[1], own, start)
    parts = exchange(parts, "ra")
    hids = kernel_call(functools.partial(hidden_kernel, features), struct((ra, 3 * TILE, hidden), bf16))(parts)
    hids = exchange(hids, "ra")
    branch = kernel_call(down_kernel, struct((z, tokens // z, width), bf16))(hids, *downs)
    return exchange(branch, "z")


def body(
    hidden_states,
    gain_first,
    gate_first,
    up_first,
    down_first,
    gain_second,
    gate_second,
    up_second,
    down_second,
    gain_last,
):
    ra, z, c = (lax.axis_size(axis) for axis in ("ra", "z", "c"))
    width = hidden_states.shape[1]
    features = width * ra
    rows = hidden_states.shape[0] // (z * c)
    struct = jax.ShapeDtypeStruct
    blocks = hidden_states.reshape(z, c, rows, width)
    stream = lax.dynamic_index_in_dim(blocks, lax.axis_index("c"), 1, keepdims=False)
    start = lax.dynamic_index_in_dim(stream, lax.axis_index("z"), 0, keepdims=False)
    pairs = []
    for w in (gate_first.T, up_first.T, down_first, gate_second.T, up_second.T, down_second):
        pairs.append((w, partner(w)))
    gains = [gain.reshape(-1, LANES) for gain in (gain_first, gain_second, gain_last)]
    parts = half_step(0, stream.reshape(z * rows, width), start, gains[0], *pairs[:3], features)
    first, start = kernel_call(update_kernel, [struct((z, rows, width), bf16), struct((rows, width), bf16)])(
        parts, start
    )
    stream = exchange(first, "z").reshape(z * rows, width)
    parts = half_step(1, stream, start, gains[1], *pairs[3:], features)
    second, squares = kernel_call(
        last_kernel, [struct((rows, width), bf16), struct((ra, TILE, LANES), f32)]
    )(parts, start)
    squares = exchange(squares, "ra")
    closed = kernel_call(functools.partial(closing_kernel, features), struct((z * c, rows, width), bf16))(
        squares, second, gains[2]
    )
    return exchange(closed, ("z", "c")).reshape(hidden_states.shape)


def solution(mesh):
    split = Mesh(mesh.devices.reshape(mesh.shape["ra"], -1, 2), ("ra", "z", "c"))
    cb = ("z", "c")
    return jax.shard_map(
        body,
        mesh=split,
        in_specs=(
            P(None, "ra"),
            P("ra"),
            P("ra", cb),
            P("ra", cb),
            P(cb, "ra"),
            P("ra"),
            P("ra", cb),
            P("ra", cb),
            P(cb, "ra"),
            P("ra"),
        ),
        out_specs=P(None, "ra"),
        check_vma=False,
    )
```
